32 devices in a mesh: ep: 8 (over z, x), tp: 4 (over y, core).
Axes of the slice: x: 2, y: 2, z: 4, core: 2. Of those that a mesh axis runs over, the one named last changes fastest.
Arguments:
- mix_values: bfloat16 [4096, 2048], P('ep', 'tp'), may hold values from -6 to 6
- mix_inner_gate: bfloat16 [4096, 2048], P('ep', 'tp'), may hold values from -6 to 6
- mix_outer_gate: bfloat16 [4096, 2048], P('ep', 'tp'), may hold values from -6 to 6
- conv_taps: bfloat16 [3, 2048], replicated, may hold values from -3 to 3
- mix_out_weight: bfloat16 [2048, 2048], P('tp'), may hold values from -0.125 to 0.125
- moe_input: bfloat16 [4096, 2048], P('ep'), may hold values from -36 to 36
- norm_gain: float32 [2048], replicated, may hold values from 0.1 to 1.9
- routes: int32 [4096, 2], P('ep'), may hold values from 0 to 7, all different within a row; in each aligned block of 128 rows (0 to 127, 128 to 255, ...) at most 64 rows name the same one
- route_weights: float32 [4096, 2], P('ep'), may hold values from 0.05 to 1
- expert_gate: bfloat16 [8, 2048, 1024], P('ep', None, 'tp'), may hold values from -0.125 to 0.125
- expert_up: bfloat16 [8, 2048, 1024], P('ep', None, 'tp'), may hold values from -0.125 to 0.125
- expert_down: bfloat16 [8, 1024, 2048], P('ep', 'tp'), may hold values from -0.1875 to 0.1875
- shared_gate: bfloat16 [2048, 1024], P(None, 'tp'), may hold values from -0.125 to 0.125
- shared_up: bfloat16 [2048, 1024], P(None, 'tp'), may hold values from -0.125 to 0.125
- shared_down: bfloat16 [1024, 2048], P('tp'), may hold values from -0.1875 to 0.1875
Outputs:
- mixed_out: bfloat16 [4096, 2048], P(('ep', 'tp'))
- expert_out: bfloat16 [4096, 2048], P(('ep', 'tp'))
The draws below stay inside these ranges and needn't reach their ends.
Inputs may be any that keep to these rules, and one draw needn't show every extreme that they name: `routes`: each row names 2 different experts; in each aligned block of 128 rows no expert is named more than 64 times, and in every draw some block names some expert exactly 64 times.
All inputs are finite; a program needn't handle non-finite values.
Results may differ from the reference program's by a relative error of at most 0.012.
Values may be sent and summed in bfloat16 or wider, within the bound.
No kernel may reach another device: no remote copies, remote signals or barrier semaphores. Data moves between devices by JAX's collectives and lax.ppermute only.
A program may use at most 128 MiB of HBM per device.

```python
import math
import jax
import jax.numpy as jnp
import numpy as np
from jax import lax

D = 2048
HID = 1024
TAPS = 3
TOP = 2
EXPERTS = 8
TOKENS_A = 4096
TOK_B = 128
TOKENS_B = 4096
CAP = 64
N_TP = 4


def draw_moe_input(key, part):
    base_key, row_key, column_key = jax.random.split(jax.random.fold_in(key, 17), 3)
    row_scale = 0.3 * jnp.exp(jax.random.uniform(row_key, (TOKENS_B, 1), jnp.float32, 0.0, math.log(10.0)))
    column_scale = 0.3 * jnp.exp(jax.random.uniform(column_key, (1, D), jnp.float32, 0.0, math.log(10.0)))
    base = jax.random.normal(base_key, (TOKENS_B, D), jnp.float32)
    return (jnp.clip(base, -4.0, 4.0) * row_scale * column_scale).astype(jnp.bfloat16)


def block_levels(key, shape, shards, smallest, top_value):
    def one(axis_at, shards_of):
        steps = jax.random.uniform(jax.random.fold_in(jax.random.fold_in(key, 6), axis_at), (shards_of,), jnp.float32, smallest / len(shards), top_value / len(shards))
        return jnp.repeat(jnp.exp(steps), shape[axis_at] // shards_of).reshape((-1,) + (1,) * (len(shape) - axis_at - 1))

    gain = one(*shards[0])
    for cut in shards[1:]:
        gain = gain * one(*cut)
    return gain


def assign_block(key, own, number, rows, number_of, top, reach, skew):
    order = jax.random.permutation(key, number_of)
    crowded, usual = shares(number_of, rows * top, reach, skew, True), shares(number_of, rows * top, reach, skew, False)
    places = jnp.arange(number_of)

    def named(tallies, turn):
        used = int((tallies > 0).sum())
        fixed = max(1, used // 4)
        shifted = fixed + (places - fixed + turn * (used - fixed)) % max(1, number_of - fixed)
        return jnp.zeros((number_of,), jnp.int32).at[order[jnp.where(places < fixed, places, shifted)]].set(jnp.asarray(tallies, jnp.int32))

    tallies = jnp.where(number % 4 == 0, named(crowded, number // 4), named(usual, number - number // 4 - 1))
    mixed = jax.random.permutation(jax.random.fold_in(own, 3), number_of)
    giver, taker = mixed[0:number_of // 2 * 2:2], mixed[1:number_of // 2 * 2:2]
    room = jnp.minimum(tallies[giver] - 1, reach - tallies[taker]) // 2
    room = jnp.where((giver == order[0]) | (taker == order[0]) | (tallies[taker] == 0), 0, jnp.maximum(room, 0))
    shifted = jax.random.randint(jax.random.fold_in(own, 4), (number_of // 2,), 0, 1 << 20) % (room + 1)
    tallies = tallies.at[giver].add(-shifted).at[taker].add(shifted)
    members = jnp.searchsorted(jnp.cumsum(tallies), jnp.arange(rows * top), side="right").astype(jnp.int32)
    table = members.reshape(top, rows).T
    table = table[jax.random.permutation(jax.random.fold_in(own, 1), rows)]
    turn = jax.random.randint(jax.random.fold_in(own, 2), (rows, 1), 0, top)
    return jnp.take_along_axis(table, (jnp.arange(top)[None, :] + turn) % top, axis=1)


def shares(count, total, most, slope, full):
    weights = [(1 << 20) // math.isqrt(rank ** slope) + 1 for rank in range(1, count + 1)]
    largest = most if full else min(most, max(-(-total // count), total * weights[0] // sum(weights)))
    least = 1 if total - largest >= count - 1 else 0
    holding, rest = [largest] + [least] * (count - 1), total - largest - least * (count - 1)
    while rest > 0:
        free = [i for i in range(1, count) if holding[i] < largest] or [i for i in range(1, count) if holding[i] < most]
        whole, remaining = sum([weights[i] for i in free]), rest
        for i in free:
            more = min(most - holding[i], max(1, remaining * weights[i] // whole), rest)
            holding[i] = holding[i] + more
            rest = rest - more
    return np.array(holding)


def gaussian(rng, extent, width, reach, cuts=(), kind=jnp.bfloat16):
    factor_of = block_levels(rng, extent, cuts, -0.22, 0.18) if cuts else 1.0
    drawn = jax.random.normal(rng, extent, jnp.float32) * width * factor_of
    return jnp.minimum(jnp.maximum(drawn, -reach), reach).astype(kind)


def setup_inputs(seed: int = 0) -> dict:
    key_list = jax.random.split(jax.random.key(seed), 16)
    mix_values = gaussian(key_list[0], (TOKENS_A, D), 1.0, 6.0, ((0, 8), (1, 4)))
    mix_inner_gate = gaussian(key_list[1], (TOKENS_A, D), 1.0, 6.0, ((0, 8), (1, 4)))
    mix_outer_gate = gaussian(key_list[2], (TOKENS_A, D), 1.0, 6.0, ((0, 8), (1, 4)))
    conv_taps = gaussian(key_list[3], (TAPS, D), 0.6, 3.0)
    mix_out_weight = gaussian(key_list[4], (D, D), D ** -0.5, 0.125, ((0, 4),))
    moe_input = draw_moe_input(jax.random.fold_in(key_list[15], 71), 0)
    norm_gain = jnp.clip(1.0 + 0.18 * jax.random.normal(key_list[6], (D,), jnp.float32), 0.1, 1.9)
    routes_keys = jax.random.split(jax.random.fold_in(key_list[7], 1), TOKENS_B // TOK_B)
    routes_turns = jax.random.permutation(jax.random.fold_in(key_list[7], 3), TOKENS_B // TOK_B)
    routes = jax.vmap(lambda own, number: assign_block(jax.random.fold_in(key_list[7], 2), own, number, TOK_B, EXPERTS, TOP, CAP, 2))(routes_keys, routes_turns).reshape((TOKENS_B, TOP))
    route_weights = jnp.clip(jnp.exp(math.log(1.0) - 2.9957323 * jax.random.uniform(key_list[8], (TOKENS_B, TOP), jnp.float32) ** block_levels(key_list[8], (TOKENS_B, TOP), ((0, 8),), -0.2, 0.2)), 0.05, 1.0)
    expert_gate = gaussian(key_list[9], (EXPERTS, D, HID), D ** -0.5, 0.125, ((0, 8), (2, 4)))
    expert_up = gaussian(key_list[10], (EXPERTS, D, HID), D ** -0.5, 0.125, ((0, 8), (2, 4)))
    expert_down = gaussian(key_list[11], (EXPERTS, HID, D), HID ** -0.5, 0.1875, ((0, 8), (1, 4)))
    shared_gate = gaussian(key_list[12], (D, HID), D ** -0.5, 0.125, ((1, 4),))
    shared_up = gaussian(key_list[13], (D, HID), D ** -0.5, 0.125, ((1, 4),))
    shared_down = gaussian(key_list[14], (HID, D), HID ** -0.5, 0.1875, ((0, 4),))
    return dict(mix_values=mix_values, mix_inner_gate=mix_inner_gate, mix_outer_gate=mix_outer_gate, conv_taps=conv_taps, mix_out_weight=mix_out_weight, moe_input=moe_input, norm_gain=norm_gain, routes=routes, route_weights=route_weights, expert_gate=expert_gate, expert_up=expert_up, expert_down=expert_down, shared_gate=shared_gate, shared_up=shared_up, shared_down=shared_down)


def dot_wide(left, right):
    return jnp.dot(left.astype(jnp.float32), right.astype(jnp.float32), preferred_element_type=jnp.float32)

def slot_table(route_block, experts, capacity):
    tokens, top = route_block.shape
    flat = route_block.reshape(-1).astype(jnp.int32)
    onehot = (flat[:, None] == jnp.arange(experts, dtype=jnp.int32)[None, :]).astype(jnp.int32)
    before = jnp.cumsum(onehot, axis=0) - onehot
    target = flat * capacity + lax.optimization_barrier(jnp.sum(before * onehot, axis=1))
    match = target[None, :] == jnp.arange(experts * capacity, dtype=jnp.int32)[:, None]
    owner = lax.optimization_barrier(jnp.sum(jnp.where(match, jnp.arange(tokens * top, dtype=jnp.int32)[None, :], 0), axis=1))
    filled = jnp.any(match, axis=1)
    return (target.reshape(tokens, top), owner.reshape(experts, capacity), filled.reshape(experts, capacity))

def rounded(values):
    return lax.optimization_barrier(values.astype(jnp.bfloat16)).astype(jnp.float32)

def reference(mix_values, mix_inner_gate, mix_outer_gate, conv_taps, mix_out_weight, moe_input, norm_gain, routes, route_weights, expert_gate, expert_up, expert_down, shared_gate, shared_up, shared_down):
    product = mix_inner_gate.astype(jnp.float32) * mix_values.astype(jnp.float32)
    length = product.shape[0]
    padded = jnp.concatenate([jnp.zeros((TAPS - 1, D), jnp.float32), product], axis=0)
    taps = conv_taps.astype(jnp.float32)
    convolved = taps[0] * padded[0:length]
    for offset in range(1, TAPS):
        convolved = convolved + taps[offset] * padded[offset:offset + length]
    gated_rows = (mix_outer_gate.astype(jnp.float32) * convolved).astype(jnp.bfloat16)
    mixed_out = dot_wide(gated_rows, mix_out_weight).astype(jnp.bfloat16)
    values = moe_input.astype(jnp.float32)
    scale = lax.rsqrt(lax.optimization_barrier(jnp.mean(values * values, axis=1, keepdims=True)) + 1e-06)
    normed = (values * scale * norm_gain).astype(jnp.bfloat16)
    part = HID // N_TP
    shared_hidden = (jax.nn.silu(dot_wide(normed, shared_gate)) * dot_wide(normed, shared_up)).astype(jnp.bfloat16)
    shared = jnp.zeros((normed.shape[0], D), jnp.float32)
    for quarter in range(N_TP):
        shared = shared + rounded(dot_wide(shared_hidden[:, quarter * part:(quarter + 1) * part], shared_down[quarter * part:(quarter + 1) * part]))
    blocks = normed.shape[0] // TOK_B
    unused, owners, filled = jax.vmap(lambda block: slot_table(block, EXPERTS, CAP))(routes.reshape(blocks, TOK_B, TOP))
    owners = owners + (jnp.arange(blocks, dtype=jnp.int32) * (TOK_B * TOP))[:, None, None]
    pairs_by_expert = owners.transpose(1, 0, 2).reshape(EXPERTS, blocks * CAP)
    valid_by_expert = filled.transpose(1, 0, 2).reshape(EXPERTS, blocks * CAP)
    mix_weights = 2.5 * route_weights / lax.optimization_barrier(jnp.sum(route_weights, axis=1, keepdims=True))
    flat_weights = mix_weights.reshape(-1)

    def per_expert(total, inputs):
        weight_gate, weight_up, weight_down, pairs, valid = inputs
        token_index = pairs // TOP
        rows = normed[token_index]
        hidden = (jax.nn.silu(dot_wide(rows, weight_gate)) * dot_wide(rows, weight_up)).astype(jnp.bfloat16)
        result = jnp.zeros((rows.shape[0], D), jnp.float32)
        for quarter in range(N_TP):
            result = result + rounded(dot_wide(hidden[:, quarter * part:(quarter + 1) * part], weight_down[quarter * part:(quarter + 1) * part]))
        result = rounded(result)
        share = jnp.where(valid, flat_weights[pairs], 0.0)
        return (total.at[token_index].add(result * share[:, None]), None)
    total, unused_out = lax.scan(per_expert, shared, (expert_gate, expert_up, expert_down, pairs_by_expert, valid_by_expert))
    return (mixed_out, total.astype(jnp.bfloat16))
```

```python
import jax
import jax.numpy as jnp
from jax import lax
from jax.sharding import PartitionSpec as P


def from_behind(value, axis, steps):
    count = lax.axis_size(axis)
    initial, last = (max(0, -steps), min(count, count - steps))
    return lax.ppermute(value, axis, [(source, source + steps) for source in range(initial, last)])


def exchange(value, axis, distance):
    count = lax.axis_size(axis)
    return lax.ppermute(value, axis, [(source, source ^ distance) for source in range(count)])


def distances(axis):
    count = lax.axis_size(axis)
    return [1 << bit for bit in range(count.bit_length() - 1)]


def gather_blocks(value, axis):
    count = lax.axis_size(axis)
    blocks = [value]
    if count & (count - 1):
        for step in range(1, count):
            pairs = [(source, (source + step) % count) for source in range(count)]
            blocks.append(lax.ppermute(value, axis, pairs))
        return blocks
    for distance in reversed(distances(axis)):
        sent = [exchange(value, axis, distance)]
        blocks = blocks + sent + [exchange(held, axis, distance) for held in blocks[1:]]
    return blocks


def add_scatter(partial, axis):
    count = lax.axis_size(axis)
    if count & (count - 1):
        return lax.psum_scatter(partial, axis, scatter_dimension=0, tiled=False).astype(jnp.float32)
    member = lax.axis_index(axis)
    held = partial
    for distance in distances(axis):
        bit = (member // distance) % 2
        pairs = held.reshape(held.shape[0] // 2, 2, *held.shape[1:])
        away = lax.dynamic_index_in_dim(pairs, 1 - bit, 1, keepdims=False)
        kept = lax.dynamic_index_in_dim(pairs, bit, 1, keepdims=False)
        summed = kept.astype(jnp.float32) + exchange(away.astype(jnp.bfloat16), axis, distance).astype(jnp.float32)
        held = summed if held.shape[0] == 2 else summed.astype(jnp.bfloat16)
    return held[0]


def slot_targets(route_block, experts, capacity):
    tokens, top = route_block.shape
    flat = route_block.reshape(-1)
    onehot = (flat[:, None] == jnp.arange(experts, dtype=jnp.int32)[None, :]).astype(jnp.int32)
    before = jnp.cumsum(onehot, axis=0) - onehot
    target = flat * capacity + jnp.sum(before * onehot, axis=1)
    return target.reshape(tokens, top)


def pick(match, rows):
    return jnp.dot(match.astype(jnp.bfloat16), rows, preferred_element_type=jnp.float32)


def on_device(
    mix_values,
    mix_inner_gate,
    mix_outer_gate,
    conv_taps,
    mix_out_weight,
    moe_input,
    norm_gain,
    routes,
    route_weights,
    expert_gate,
    expert_up,
    expert_down,
    shared_gate,
    shared_up,
    shared_down,
):
    parts = lax.axis_size("tp")
    member = lax.axis_index("tp")
    groups = lax.axis_size("ep")
    rows_here, width_here = mix_values.shape
    reach = conv_taps.shape[0] - 1
    all_gate = gather_blocks(expert_gate, "tp")
    all_up = gather_blocks(expert_up, "tp")
    all_down = gather_blocks(expert_down, "tp")
    taps = lax.dynamic_slice_in_dim(conv_taps, member * width_here, width_here, 1).astype(
        jnp.float32
    )
    boundary = from_behind(
        jnp.stack([mix_values[rows_here - reach :], mix_inner_gate[rows_here - reach :]]), "ep", 1
    )
    product = jnp.concatenate(
        [
            boundary[1].astype(jnp.float32) * boundary[0].astype(jnp.float32),
            mix_inner_gate.astype(jnp.float32) * mix_values.astype(jnp.float32),
        ],
        axis=0,
    )
    convolved = taps[0] * product[0:rows_here]
    for offset in range(1, reach + 1):
        convolved = convolved + taps[offset] * product[offset : offset + rows_here]
    gated_rows = (mix_outer_gate.astype(jnp.float32) * convolved).astype(jnp.bfloat16)
    mixed_part = jnp.dot(
        gated_rows, mix_out_weight, preferred_element_type=jnp.float32
    ).astype(jnp.bfloat16)
    local_experts = expert_gate.shape[0]
    experts = local_experts * groups
    width = moe_input.shape[1]
    block = moe_input.shape[0] // parts
    top = routes.shape[1]
    capacity = 2 * block * top // experts
    values = moe_input.astype(jnp.float32)
    scale = lax.rsqrt(jnp.mean(values * values, axis=1, keepdims=True) + 1e-06)
    normed_all = (values * scale * norm_gain).astype(jnp.bfloat16)
    own_weights = lax.dynamic_slice_in_dim(route_weights, member * block, block, 0)
    shared_gate_part = jnp.dot(normed_all, shared_gate, preferred_element_type=jnp.float32)
    shared_up_part = jnp.dot(normed_all, shared_up, preferred_element_type=jnp.float32)
    hidden_shared = (jax.nn.silu(shared_gate_part) * shared_up_part).astype(jnp.bfloat16)
    shared_part = jnp.dot(
        hidden_shared, shared_down, preferred_element_type=jnp.float32
    ).astype(jnp.bfloat16)
    mixed = add_scatter(
        mixed_part.reshape(parts, block, mixed_part.shape[1]), "tp"
    ).astype(jnp.bfloat16)
    shared_own = add_scatter(shared_part.reshape(parts, block, width), "tp")
    own_routes = lax.dynamic_slice_in_dim(routes, member * block, block, 0)
    own_target = slot_targets(own_routes, experts, capacity)
    slots = jnp.arange(experts * capacity, dtype=jnp.int32)
    own_rows = lax.dynamic_slice_in_dim(normed_all, member * block, block, 0)
    holds = own_target[None, :, 0] == slots[:, None]
    for slot_number in range(1, top):
        holds = holds | (own_target[None, :, slot_number] == slots[:, None])
    arrived = lax.all_to_all(
        pick(holds, own_rows).astype(jnp.bfloat16).reshape(experts, capacity, width),
        "ep",
        split_axis=0,
        concat_axis=0,
        tiled=True,
    )
    routed_rows = groups * capacity
    rows = arrived.reshape(groups, local_experts, capacity, width)
    results = []
    for local in range(local_experts):
        mine = rows[:, local].reshape(routed_rows, width)
        hidden = []
        for part in range(parts):
            gate_part = jnp.dot(mine, all_gate[part][local], preferred_element_type=jnp.float32)
            up_part = jnp.dot(mine, all_up[part][local], preferred_element_type=jnp.float32)
            hidden.append((jax.nn.silu(gate_part) * up_part).astype(jnp.bfloat16))
        result = jnp.dot(
            jnp.concatenate(hidden, axis=1),
            jnp.concatenate([held[local] for held in all_down], axis=0),
            preferred_element_type=jnp.float32,
        )
        results.append(result.astype(jnp.bfloat16).reshape(groups, 1, capacity, width))
    routed_back = (results[0] if local_experts == 1 else jnp.concatenate(results, axis=1)).reshape(
        groups, local_experts * capacity, width
    )
    returned = lax.all_to_all(routed_back, "ep", split_axis=0, concat_axis=0, tiled=True).reshape(
        experts * capacity, width
    )
    mix_weights = 2.5 * own_weights / jnp.sum(own_weights, axis=1, keepdims=True)
    total = shared_own
    for slot_number in range(top):
        chosen = pick(own_target[:, slot_number : slot_number + 1] == slots[None, :], returned)
        total = total + mix_weights[:, slot_number : slot_number + 1] * chosen
    expert_out = total.astype(jnp.bfloat16)
    return (mixed, expert_out)


def solution(mesh):
    return jax.shard_map(
        on_device,
        mesh=mesh,
        in_specs=(
            P("ep", "tp"),
            P("ep", "tp"),
            P("ep", "tp"),
            P(),
            P("tp", None),
            P("ep", None),
            P(),
            P("ep", None),
            P("ep", None),
            P("ep", None, "tp"),
            P("ep", None, "tp"),
            P("ep", "tp", None),
            P(None, "tp"),
            P(None, "tp"),
            P("tp", None),
        ),
        out_specs=(P(("ep", "tp"), None), P(("ep", "tp"), None)),
        check_vma=False,
    )
```

```python
import jax
import jax.numpy as jnp
from jax import lax
from jax.experimental import pallas as pl
from jax.experimental.pallas import tpu as pltpu
from jax.sharding import PartitionSpec as P


def from_behind(value, axis, steps):
    count = lax.axis_size(axis)
    initial, last = (max(0, -steps), min(count, count - steps))
    return lax.ppermute(value, axis, [(source, source + steps) for source in range(initial, last)])


def exchange(value, axis, distance):
    count = lax.axis_size(axis)
    return lax.ppermute(value, axis, [(source, source ^ distance) for source in range(count)])


def distances(axis):
    count = lax.axis_size(axis)
    return [1 << bit for bit in range(count.bit_length() - 1)]


def gather_blocks(value, axis):
    count = lax.axis_size(axis)
    blocks = [value]
    if count & (count - 1):
        for step in range(1, count):
            pairs = [(source, (source + step) % count) for source in range(count)]
            blocks.append(lax.ppermute(value, axis, pairs))
        return blocks
    for distance in reversed(distances(axis)):
        sent = [exchange(value, axis, distance)]
        blocks = blocks + sent + [exchange(held, axis, distance) for held in blocks[1:]]
    return blocks


def add_scatter(partial, axis):
    count = lax.axis_size(axis)
    if count & (count - 1):
        return lax.psum_scatter(partial, axis, scatter_dimension=0, tiled=False).astype(jnp.float32)
    member = lax.axis_index(axis)
    held = partial
    for distance in distances(axis):
        bit = (member // distance) % 2
        pairs = held.reshape(held.shape[0] // 2, 2, *held.shape[1:])
        away = lax.dynamic_index_in_dim(pairs, 1 - bit, 1, keepdims=False)
        kept = lax.dynamic_index_in_dim(pairs, bit, 1, keepdims=False)
        summed = kept.astype(jnp.float32) + exchange(away.astype(jnp.bfloat16), axis, distance).astype(jnp.float32)
        held = summed if held.shape[0] == 2 else summed.astype(jnp.bfloat16)
    return held[0]


def slot_targets(route_block, experts, capacity):
    tokens, top = route_block.shape
    flat = route_block.reshape(-1)
    onehot = (flat[:, None] == jnp.arange(experts, dtype=jnp.int32)[None, :]).astype(jnp.int32)
    before = jnp.cumsum(onehot, axis=0) - onehot
    target = flat * capacity + jnp.sum(before * onehot, axis=1)
    return target.reshape(tokens, top)


def pick(match, rows):
    return jnp.dot(match.astype(jnp.bfloat16), rows, preferred_element_type=jnp.float32)


def expert_body(*refs):
    rows, out = refs[0], refs[-1]
    parts = (len(refs) - 2) // 3
    gates, ups, downs = refs[1 : 1 + parts], refs[1 + parts : 1 + 2 * parts], refs[1 + 2 * parts : -1]
    total = None
    for gate, up, down in zip(gates, ups, downs):
        gate_part = jnp.dot(rows[...], gate[...], preferred_element_type=jnp.float32)
        up_part = jnp.dot(rows[...], up[...], preferred_element_type=jnp.float32)
        hidden = (gate_part / (1.0 + jnp.exp(-gate_part)) * up_part).astype(jnp.bfloat16)
        result = jnp.dot(hidden, down[...], preferred_element_type=jnp.float32)
        total = result if total is None else total + result
    out[...] = total.astype(jnp.bfloat16)


def run_expert(rows, gates, ups, downs):
    return pl.pallas_call(
        expert_body,
        out_shape=jax.ShapeDtypeStruct((rows.shape[0], downs[0].shape[1]), jnp.bfloat16),
        compiler_params=pltpu.CompilerParams(vmem_limit_bytes=56 * 1024 * 1024),
    )(rows, *gates, *ups, *downs)


def on_device(
    mix_values,
    mix_inner_gate,
    mix_outer_gate,
    conv_taps,
    mix_out_weight,
    moe_input,
    norm_gain,
    routes,
    route_weights,
    expert_gate,
    expert_up,
    expert_down,
    shared_gate,
    shared_up,
    shared_down,
):
    parts = lax.axis_size("tp")
    member = lax.axis_index("tp")
    groups = lax.axis_size("ep")
    rows_here, width_here = mix_values.shape
    reach = conv_taps.shape[0] - 1
    all_gate = gather_blocks(expert_gate, "tp")
    all_up = gather_blocks(expert_up, "tp")
    all_down = gather_blocks(expert_down, "tp")
    taps = lax.dynamic_slice_in_dim(conv_taps, member * width_here, width_here, 1).astype(
        jnp.float32
    )
    boundary = from_behind(
        jnp.stack([mix_values[rows_here - reach :], mix_inner_gate[rows_here - reach :]]), "ep", 1
    )
    product = jnp.concatenate(
        [
            boundary[1].astype(jnp.float32) * boundary[0].astype(jnp.float32),
            mix_inner_gate.astype(jnp.float32) * mix_values.astype(jnp.float32),
        ],
        axis=0,
    )
    convolved = taps[0] * product[0:rows_here]
    for offset in range(1, reach + 1):
        convolved = convolved + taps[offset] * product[offset : offset + rows_here]
    gated_rows = (mix_outer_gate.astype(jnp.float32) * convolved).astype(jnp.bfloat16)
    mixed_part = jnp.dot(
        gated_rows, mix_out_weight, preferred_element_type=jnp.float32
    ).astype(jnp.bfloat16)
    local_experts = expert_gate.shape[0]
    experts = local_experts * groups
    width = moe_input.shape[1]
    block = moe_input.shape[0] // parts
    top = routes.shape[1]
    capacity = 2 * block * top // experts
    values = moe_input.astype(jnp.float32)
    scale = lax.rsqrt(jnp.mean(values * values, axis=1, keepdims=True) + 1e-06)
    normed_all = (values * scale * norm_gain).astype(jnp.bfloat16)
    own_weights = lax.dynamic_slice_in_dim(route_weights, member * block, block, 0)
    shared_gate_part = jnp.dot(normed_all, shared_gate, preferred_element_type=jnp.float32)
    shared_up_part = jnp.dot(normed_all, shared_up, preferred_element_type=jnp.float32)
    hidden_shared = (jax.nn.silu(shared_gate_part) * shared_up_part).astype(jnp.bfloat16)
    shared_part = jnp.dot(
        hidden_shared, shared_down, preferred_element_type=jnp.float32
    ).astype(jnp.bfloat16)
    mixed = add_scatter(
        mixed_part.reshape(parts, block, mixed_part.shape[1]), "tp"
    ).astype(jnp.bfloat16)
    shared_own = add_scatter(shared_part.reshape(parts, block, width), "tp")
    own_routes = lax.dynamic_slice_in_dim(routes, member * block, block, 0)
    own_target = slot_targets(own_routes, experts, capacity)
    slots = jnp.arange(experts * capacity, dtype=jnp.int32)
    own_rows = lax.dynamic_slice_in_dim(normed_all, member * block, block, 0)
    holds = own_target[None, :, 0] == slots[:, None]
    for slot_number in range(1, top):
        holds = holds | (own_target[None, :, slot_number] == slots[:, None])
    arrived = lax.all_to_all(
        pick(holds, own_rows).astype(jnp.bfloat16).reshape(experts, capacity, width),
        "ep",
        split_axis=0,
        concat_axis=0,
        tiled=True,
    )
    routed_rows = groups * capacity
    rows = arrived.reshape(groups, local_experts, capacity, width)
    results = []
    for local in range(local_experts):
        mine = rows[:, local].reshape(routed_rows, width)
        result = run_expert(
            mine,
            [held[local] for held in all_gate],
            [held[local] for held in all_up],
            [held[local] for held in all_down],
        )
        results.append(result.reshape(groups, 1, capacity, width))
    routed_back = (results[0] if local_experts == 1 else jnp.concatenate(results, axis=1)).reshape(
        groups, local_experts * capacity, width
    )
    returned = lax.all_to_all(routed_back, "ep", split_axis=0, concat_axis=0, tiled=True).reshape(
        experts * capacity, width
    )
    mix_weights = 2.5 * own_weights / jnp.sum(own_weights, axis=1, keepdims=True)
    total = shared_own
    for slot_number in range(top):
        chosen = pick(own_target[:, slot_number : slot_number + 1] == slots[None, :], returned)
        total = total + mix_weights[:, slot_number : slot_number + 1] * chosen
    expert_out = total.astype(jnp.bfloat16)
    return (mixed, expert_out)


def solution(mesh):
    return jax.shard_map(
        on_device,
        mesh=mesh,
        in_specs=(
            P("ep", "tp"),
            P("ep", "tp"),
            P("ep", "tp"),
            P(),
            P("tp", None),
            P("ep", None),
            P(),
            P("ep", None),
            P("ep", None),
            P("ep", None, "tp"),
            P("ep", None, "tp"),
            P("ep", "tp", None),
            P(None, "tp"),
            P(None, "tp"),
            P("tp", None),
        ),
        out_specs=(P(("ep", "tp"), None), P(("ep", "tp"), None)),
        check_vma=False,
    )
```
